32 devices in a mesh: grp: 2 (over y), dp: 2 (over x), kv: 4 (over z), tp: 2 (over core).
Axes of the slice: x: 2, y: 2, z: 4, core: 2. Of those that a mesh axis runs over, the one named last changes fastest.
Arguments:
- hidden_in: bfloat16 [4, 1024, 2048], P(('grp', 'dp'), 'kv', 'tp'), parts along dimension 0, may hold values from -45 to 45
- norm_gain: float32 [2048], P('tp'), may hold values from 0.1 to 1.9
- query_weight: bfloat16 [2048, 1024], P('kv', 'tp'), may hold values from -1 to 1
- key_weight: bfloat16 [2048, 256], P('kv', 'tp'), may hold values from -60 to 60
- value_weight: bfloat16 [2048, 256], P('kv', 'tp'), may hold values from -0.125 to 0.125
- out_weight: bfloat16 [2048, 1024], P('kv', 'tp'), may hold values from -0.1875 to 0.1875
- slopes: float32 [8], P('tp'), may hold values from 0 to 3
- block_choice: int32 [4, 16, 16], P(('grp', 'dp'), 'kv'), parts along dimension 0, may hold values from 0 to 15, as said below
Outputs:
- mixed: bfloat16 [4, 1024, 2048], P(('grp', 'dp'), ('kv', 'tp')), parts along dimension 0
The draws below stay inside these ranges and needn't reach their ends.
There are 2 independent parts, one for each index of `grp`. The reference program is written for one: setup_inputs(seed, part) draws one part's arguments, and reference() takes and returns one part's arrays. A program takes and returns all parts, laid end to end along the dimension named above; an argument that names none is the same for every part. Nothing has to cross between parts.
Inputs may be any that keep to these rules, and one draw needn't show every extreme that they name: `block_choice`: for query block i the entries name key blocks 0 to i; the first min(16, i + 1) entries are distinct and include block i; any later entries equal i.
All inputs are finite; a program needn't handle non-finite values.
Results may differ from the reference program's by a relative error of at most 0.0092.
Values may be sent and summed in bfloat16 or wider, within the bound.
A program may use at most 64 MiB of HBM per device.

```python
import jax
import jax.numpy as jnp
from jax import lax

D = 2048
HEADS = 8
KV_HEADS = 2
HEAD_DIM = 128
BLOCK = 64
NSEL = 16
SEQS = 2
LEN = 1024
NBLK = 16
N_TP = 2


def draw_hidden_in(key, part):
    base_key = jax.random.fold_in(key, 21)
    scale_key = jax.random.fold_in(key, 22)
    base = jnp.clip(jax.random.normal(base_key, (SEQS, LEN, D), jnp.float32), -6.0, 6.0)
    scales = jnp.exp(jax.random.uniform(scale_key, (SEQS, LEN, 2), jnp.float32, -2.0, 2.0))
    return (base * jnp.repeat(scales, D // 2, axis=2)).astype(jnp.bfloat16)


def projection_pair(key):
    query_key = jax.random.fold_in(key, 11)
    fresh_key = jax.random.fold_in(key, 12)
    query = jnp.clip(jax.random.normal(query_key, (D, HEADS * HEAD_DIM), jnp.float32), -5.0, 5.0) * D ** (-0.5)
    fresh = jnp.clip(jax.random.normal(fresh_key, (D, KV_HEADS, HEAD_DIM), jnp.float32), -5.0, 5.0) * D ** (-0.5)
    keys = fresh
    return (query, keys.reshape(D, KV_HEADS * HEAD_DIM))


def draw_query_weight(key, part):
    return projection_pair(key)[0].astype(jnp.bfloat16)


def draw_key_weight(key, part):
    return projection_pair(key)[1].astype(jnp.bfloat16)


def draw_slopes(key, part):
    pick_key = jax.random.fold_in(key, 31)
    rate_key = jax.random.fold_in(key, 32)
    share = 0.5
    fast = jax.random.uniform(pick_key, (HEADS,), jnp.float32) < share
    unit = jax.random.uniform(rate_key, (HEADS,), jnp.float32, 0.0, 1.0)
    slow_rate = jnp.exp(jnp.log(0.05 / NBLK) + unit * jnp.log(40.0))
    fast_rate = jnp.exp(unit * jnp.log(3.0))
    return jnp.where(fast, fast_rate, slow_rate).astype(jnp.float32)


def draw_block_choice(key, part):
    noise_key = jax.random.fold_in(key, 41)
    hot_key = jax.random.fold_in(key, 42)
    query_block = jnp.arange(NBLK, dtype=jnp.int32)[:, None]
    key_block = jnp.arange(NBLK, dtype=jnp.int32)[None, :]
    noise = jax.random.randint(noise_key, (SEQS, NBLK, NBLK), 0, 65536, dtype=jnp.int32)
    hot = (jax.random.randint(hot_key, (SEQS, 1, NBLK), 0, 8, dtype=jnp.int32) == 0).astype(jnp.int32)
    forced = ((key_block == query_block) | (key_block == query_block - 1) | (key_block == query_block - NBLK // 2)).astype(jnp.int32)
    score = noise + 65536 * hot + 131072 * forced[None]
    score = jnp.where((key_block <= query_block)[None], score, -1)
    ranked = score * NBLK + key_block[None]
    unused, picked = lax.top_k(ranked, NSEL)
    count = jnp.minimum(NSEL, query_block + 1)
    slot = jnp.arange(NSEL, dtype=jnp.int32)[None, :]
    picked = jnp.where((slot < count)[None], picked, query_block[None])
    return picked.astype(jnp.int32)


def level_of(rng, extent, shards, least, high):
    def one(dim, shards_of):
        draws = jax.random.uniform(jax.random.fold_in(jax.random.fold_in(rng, 6), dim), (shards_of,), jnp.float32, least / len(shards), high / len(shards))
        return jnp.repeat(jnp.exp(draws), extent[dim] // shards_of).reshape((-1,) + (1,) * (len(extent) - dim - 1))

    gain = one(*shards[0])
    for cut in shards[1:]:
        gain = gain * one(*cut)
    return gain


def bell_draw(own_key, extent, deviation, bound, shards=(), held_as=jnp.bfloat16):
    level = level_of(own_key, extent, shards, -0.22, 0.18) if shards else 1.0
    entries = jax.random.normal(own_key, extent, jnp.float32) * deviation * level
    return jnp.minimum(jnp.maximum(entries, -bound), bound).astype(held_as)


def setup_inputs(seed: int = 0, part: int = 0) -> dict:
    splits = jax.random.split(jax.random.key(seed), 9)
    part_keys = jax.random.split(jax.random.fold_in(splits[8], part), 9)
    return {
        "hidden_in": draw_hidden_in(jax.random.fold_in(jax.random.fold_in(splits[8], part), 71), part),
        "norm_gain": jnp.clip(1.0 + 0.18 * jax.random.normal(splits[1], (D,), jnp.float32), 0.1, 1.9),
        "query_weight": draw_query_weight(jax.random.fold_in(splits[8], 71), part),
        "key_weight": draw_key_weight(jax.random.fold_in(splits[8], 71), part),
        "value_weight": bell_draw(splits[4], (D, KV_HEADS * HEAD_DIM), D ** -0.5, 0.125, ((0, 4), (1, 2))),
        "out_weight": bell_draw(splits[5], (D, HEADS * HEAD_DIM), (HEADS * HEAD_DIM) ** -0.5, 0.1875, ((0, 4), (1, 2))),
        "slopes": draw_slopes(jax.random.fold_in(splits[8], 71), part),
        "block_choice": draw_block_choice(jax.random.fold_in(jax.random.fold_in(splits[8], part), 71), part),
    }


EPS = 1e-06
NEG = -1e+30

def attend(queries, keys, values, slopes, choice):
    group = HEADS // KV_HEADS
    q_blocks = queries.reshape(NBLK, BLOCK, KV_HEADS, group, HEAD_DIM).astype(jnp.float32)
    key_blocks = keys.reshape(NBLK, BLOCK, KV_HEADS, HEAD_DIM)
    value_blocks = values.reshape(NBLK, BLOCK, KV_HEADS, HEAD_DIM)
    key_sel = key_blocks[choice].reshape(NBLK, NSEL * BLOCK, KV_HEADS, HEAD_DIM).astype(jnp.float32)
    value_sel = value_blocks[choice].reshape(NBLK, NSEL * BLOCK, KV_HEADS, HEAD_DIM).astype(jnp.float32)
    scores = jnp.einsum('nqkgd,nskd->nqkgs', q_blocks, key_sel) * HEAD_DIM ** (-0.5)
    qpos = jnp.arange(LEN, dtype=jnp.int32).reshape(NBLK, BLOCK)
    kpos = (choice[:, :, None] * BLOCK + jnp.arange(BLOCK, dtype=jnp.int32)[None, None, :]).reshape(NBLK, NSEL * BLOCK)
    dist = jnp.abs(qpos[:, :, None] - kpos[:, None, :]).astype(jnp.float32) / BLOCK
    slope_grid = slopes.reshape(KV_HEADS, group)
    scores = scores - slope_grid[None, None, :, :, None] * dist[:, :, None, None, :]
    count = jnp.minimum(NSEL, jnp.arange(NBLK, dtype=jnp.int32) + 1)
    live = jnp.arange(NSEL, dtype=jnp.int32)[None, :] < count[:, None]
    live = jnp.repeat(live, BLOCK, axis=1)[:, None, None, None, :]
    scores = jnp.where(live, scores, NEG)
    best = lax.optimization_barrier(jnp.max(scores, axis=4, keepdims=True))
    weights = jnp.where(live, jnp.exp(scores - best), 0.0)
    total = lax.optimization_barrier(jnp.sum(weights, axis=4))
    rounded = lax.optimization_barrier(weights.astype(jnp.bfloat16)).astype(jnp.float32)
    summed = jnp.einsum('nqkgs,nskd->nqkgd', rounded, value_sel)
    attended = (summed / total[..., None]).astype(jnp.bfloat16)
    return attended.reshape(LEN, HEADS * HEAD_DIM)

def reference(hidden_in, norm_gain, query_weight, key_weight, value_weight, out_weight, slopes, block_choice):
    values_in = hidden_in.astype(jnp.float32)
    mean_square = lax.optimization_barrier(jnp.mean(values_in * values_in, axis=-1, keepdims=True))
    normed = (values_in * lax.rsqrt(mean_square + EPS) * norm_gain).astype(jnp.bfloat16)

    def one(item):
        rows, choice = item
        queries = jnp.dot(rows, query_weight, preferred_element_type=jnp.float32).astype(jnp.bfloat16)
        keys = jnp.dot(rows, key_weight, preferred_element_type=jnp.float32).astype(jnp.bfloat16)
        values = jnp.dot(rows, value_weight, preferred_element_type=jnp.float32).astype(jnp.bfloat16)
        return attend(queries, keys, values, slopes, choice)
    attended = lax.map(one, (normed, block_choice)).reshape(SEQS * LEN, HEADS * HEAD_DIM)
    width = HEADS * HEAD_DIM // N_TP
    mixed = jnp.zeros((SEQS * LEN, D), jnp.float32)
    for half in range(N_TP):
        cols = attended[:, half * width:(half + 1) * width]
        weight = out_weight[:, half * width:(half + 1) * width]
        part = jnp.dot(cols, weight.T, preferred_element_type=jnp.float32).astype(jnp.bfloat16)
        mixed = mixed + lax.optimization_barrier(part).astype(jnp.float32)
    return mixed.astype(jnp.bfloat16).reshape(SEQS, LEN, D)
```

```python
import functools

import jax
import jax.numpy as jnp
from jax import lax
from jax.experimental import pallas as pl
from jax.experimental.pallas import tpu as pltpu
from jax.sharding import PartitionSpec as P

HEAD_DIM = 128
BLOCK = 64
NSEL = 16
EPS = 1e-06
NEG = -1e30
MESH = pl.DeviceIdType.MESH
BF16 = jnp.bfloat16
F32 = jnp.float32


def dot(a, b):
    return jnp.dot(a, b, preferred_element_type=F32)


def dot_t(a, b):
    return lax.dot_general(a, b, (((1,), (1,)), ((), ())), preferred_element_type=F32)


def loop(low, high, body):
    if high - low <= 4:
        for i in range(low, high):
            body(i)
    else:
        lax.fori_loop(low, high, lambda i, c: (body(i), c)[1], 0)


def kernel(n, masked, *refs):
    refs = list(refs)
    hid, gain, wq, wk, wv, wo, slopes = refs[:7]
    refs = refs[7:]
    mask = refs.pop(0) if masked else None
    (
        out, hid2, gain2, xn, fq, fk, fv, fo, qacc, kacc, vacc, qs, kall, vall,
        mrun, lrun, acc, att, pown, psend, precv,
        wsend, wrecv, ksend, krecv, hsend, hrecv, osend, orecv,
    ) = refs
    grp, dp = lax.axis_index("grp"), lax.axis_index("dp")
    z, tp = lax.axis_index("kv"), lax.axis_index("tp")
    xb, yb = lax.rem(dp, 2), lax.rem(grp, 2)
    col = 2 * yb + xb
    col_x, col_y, col_d = 2 * yb + 1 - xb, 2 * (1 - yb) + xb, 2 * (1 - yb) + 1 - xb
    x_id = (grp, dp + 1 - 2 * xb, z, tp)
    y_id = (grp + 1 - 2 * yb, dp, z, tp)
    sib = (grp, dp, z, 1 - tp)

    def at_z(other):
        return (grp, dp, other, tp)

    tokens, half_d = hid.shape
    heads = slopes.shape[0]
    rows = xn.shape[2]
    groups = (((wk, fk, 0), (wv, fv, 1)), ((wq, fq, 2),), ((wo, fo, 3),))

    barrier = pltpu.get_barrier_semaphore()
    for dev in (sib, x_id, y_id):
        pl.semaphore_signal(barrier, inc=1, device_id=dev, device_id_type=MESH)
    for d in range(1, n):
        pl.semaphore_signal(barrier, inc=1, device_id=at_z(lax.rem(z + d, n)), device_id_type=MESH)
    pl.semaphore_wait(barrier, n + 2)

    def remote(src, dst, send, recv, dev):
        return pltpu.make_async_remote_copy(
            src_ref=src, dst_ref=dst, send_sem=send, recv_sem=recv, device_id=dev, device_id_type=MESH
        )

    swap = [
        remote(hid, hid2, hsend.at[0], hrecv.at[0], sib),
        remote(gain, gain2, hsend.at[1], hrecv.at[1], sib),
    ]
    for copy in swap:
        copy.start()

    def along(shard, origin, kind, own):
        w, f, a = shard
        part = pl.ds(2 * col, 2)
        src = w.at[part] if own else f.at[origin, part]
        dev = at_z(z + 1) if kind == 0 else at_z(z - 1)
        return remote(src, f.at[origin, part], wsend.at[a, kind, origin], wrecv.at[a, 0, origin], dev)

    def across(shard, origin, kind):
        _, f, a = shard
        part, dev = {
            2: (pl.ds(2 * col, 2), x_id),
            3: (pl.ds(2 * col, 2), y_id),
            4: (pl.ds(2 * col_x, 1), y_id),
            5: (pl.ds(2 * col_y + 1, 1), x_id),
        }[kind]
        ref = f.at[origin, part]
        return remote(ref, ref, wsend.at[a, kind, origin], wrecv.at[a, kind, origin], dev)

    def arrive(shard, origin, kind):
        _, f, a = shard
        part = {
            0: pl.ds(2 * col, 2),
            2: pl.ds(2 * col_x, 2),
            3: pl.ds(2 * col_y, 2),
            4: pl.ds(2 * col_d, 1),
            5: pl.ds(2 * col_d + 1, 1),
        }[kind]
        ref = f.at[origin, part]
        remote(ref, ref, wsend.at[a, kind, origin], wrecv.at[a, kind, origin], x_id).wait_recv()

    def start_own(g):
        for shard in groups[g]:
            @pl.when(z + 1 < n)
            def _():
                along(shard, z, 0, True).start()

            @pl.when(z >= 1)
            def _():
                along(shard, z, 1, True).start()

    def both(d, body):
        @pl.when(z - d >= 0)
        def _():
            body(z - d, True)

        @pl.when(z + d < n)
        def _():
            body(z + d, False)

    def step_a(g, d):
        def body(origin, up):
            for shard in groups[g]:
                arrive(shard, origin, 0)
                if up:
                    @pl.when(z + 1 < n)
                    def _():
                        along(shard, origin, 0, False).start()
                else:
                    @pl.when(z >= 1)
                    def _():
                        along(shard, origin, 1, False).start()
                across(shard, origin, 2).start()
                across(shard, origin, 3).start()

        both(d, body)

    def step_b(g, d):
        def body(origin, up):
            for shard in groups[g]:
                arrive(shard, origin, 2)
                across(shard, origin, 4).start()
                arrive(shard, origin, 3)
                across(shard, origin, 5).start()

        both(d, body)

    def whole(f, origin):
        return f[origin].reshape(rows, f.shape[-1])

    def step_c(g, d):
        def body(origin, up):
            for shard in groups[g]:
                arrive(shard, origin, 4)
                arrive(shard, origin, 5)
                if g < 2:
                    target = (kacc, vacc, qacc)[shard[2]]
                    target[...] += dot(xn[origin], whole(shard[1], origin))
                else:
                    project_out(origin, whole(fo, origin))

        both(d, body)

    start_own(0)
    start_own(1)

    for copy in swap:
        copy.wait()
    lanes = HEAD_DIM
    square = jnp.zeros((tokens, lanes), F32)
    for ref in (hid, hid2):
        for j in range(half_d // lanes):
            piece = ref[:, j * lanes : (j + 1) * lanes].astype(F32)
            square = square + piece * piece
    inverse = lax.rsqrt(jnp.sum(square, axis=1, keepdims=True) / (2 * half_d) + EPS)
    for ref, g_ref, half in ((hid, gain, tp), (hid2, gain2, 1 - tp)):
        for j in range(half_d // lanes):
            piece = ref[:, j * lanes : (j + 1) * lanes].astype(F32)
            value = (piece * inverse * g_ref[j : j + 1, :]).astype(BF16)
            first = j * lanes
            xn[half * (n // 2) + first // rows, :, first % rows : first % rows + lanes] = value

    mine = xn[z]
    kacc[...] = dot(mine, wk[...].reshape(rows, -1))
    vacc[...] = dot(mine, wv[...].reshape(rows, -1))
    qacc[...] = dot(mine, wq[...].reshape(rows, -1))

    def key_copy(ref, i, d):
        return remote(ref.at[z], ref.at[z], ksend.at[i, d], krecv.at[i, z], at_z(z + d))

    def key_each(d, act):
        @pl.when(z + d < n)
        def _():
            for i, ref in enumerate((kall, vall)):
                act(key_copy(ref, i, d))

    def pipe(d):
        step_a(0, d)
        if isinstance(d, int):
            if d > 1:
                step_b(0, d - 1)
            if d > 2:
                step_c(0, d - 2)
        else:
            pl.when(d > 1)(lambda: step_b(0, d - 1))
            pl.when(d > 2)(lambda: step_c(0, d - 2))

    loop(1, n, pipe)
    step_a(1, 1)
    step_b(0, n - 1)
    step_c(0, n - 2)
    step_a(1, 2)
    step_b(1, 1)
    step_c(0, n - 1)
    kall[z] = kacc[...].astype(BF16)
    vall[z] = vacc[...].astype(BF16)
    loop(1, n, lambda d: key_each(d, lambda copy: copy.start()))
    start_own(2)

    def pipe_q(d):
        step_a(1, d)
        step_b(1, d - 1)
        step_c(1, d - 2)

    loop(3, n, pipe_q)
    step_b(1, n - 1)
    step_c(1, n - 2)
    step_c(1, n - 1)
    for h in range(heads):
        qs[h] = qacc[:, h * HEAD_DIM : (h + 1) * HEAD_DIM].astype(BF16)

    scale = HEAD_DIM**-0.5
    qpos = lax.broadcasted_iota(jnp.int32, (tokens, tokens), 0)
    kpos = lax.broadcasted_iota(jnp.int32, (tokens, tokens), 1)

    def chunk(d, first):
        origin = z - d
        if not first:
            for i, ref in enumerate((kall, vall)):
                remote(ref.at[origin], ref.at[origin], ksend.at[i, d], krecv.at[i, origin], sib).wait_recv()
        keys, values = kall[origin], vall[origin]
        dist = jnp.abs(qpos - kpos + d * tokens).astype(F32) / BLOCK
        for h in range(heads):
            s = dot_t(qs[h], keys) * scale - slopes[h] * dist
            if masked:
                s = s + mask[origin]
            elif first:
                s = jnp.where(kpos // BLOCK <= qpos // BLOCK, s, NEG)
            top = jnp.max(s, axis=1, keepdims=True)
            if not first:
                before = mrun[h][:, :1]
                top = jnp.maximum(top, before)
                fade = jnp.exp(before - top)
            w = jnp.exp(s - top)
            total = jnp.sum(w, axis=1, keepdims=True)
            summed = dot(w.astype(BF16), values)
            if not first:
                total = total + lrun[h][:, :1] * fade
                summed = summed + acc[h] * fade
            mrun[h] = jnp.broadcast_to(top, (tokens, HEAD_DIM))
            lrun[h] = jnp.broadcast_to(total, (tokens, HEAD_DIM))
            acc[h] = summed

    def later(d):
        pl.when(z - d >= 0)(lambda: chunk(d, False))
        step_a(2, d)
        if isinstance(d, int):
            if d > 1:
                step_b(2, d - 1)
        else:
            pl.when(d > 1)(lambda: step_b(2, d - 1))

    chunk(0, True)
    loop(1, n, later)
    step_b(2, n - 1)
    half = tokens // 2
    for h in range(heads):
        value = (acc[h] / lrun[h]).astype(BF16)
        att[:, :, h * HEAD_DIM : (h + 1) * HEAD_DIM] = value.reshape(2, half, HEAD_DIM)

    def out_copy(origin):
        return remote(psend.at[origin], precv.at[origin], osend.at[origin], orecv.at[origin], sib)

    def project_out(origin, weight):
        psend[origin] = dot_t(att[1 - tp], weight).astype(BF16)
        out_copy(origin).start()
        pown[origin] = dot_t(att[tp], weight).astype(BF16)

    project_out(z, wo[...].reshape(rows, -1))
    loop(1, n, lambda d: step_c(2, d))

    def finish(origin):
        out_copy(origin).wait()
        value = pown[origin].astype(F32) + precv[origin].astype(F32)
        first = origin * rows
        if not isinstance(origin, int):
            first = pl.multiple_of(first, rows)
        out[:, pl.ds(first, rows)] = value.astype(BF16)

    finish(z)
    loop(1, n, lambda d: both(d, lambda origin, up: finish(origin)))

    loop(1, n, lambda d: key_each(d, lambda copy: copy.wait_send()))
    for g in range(3):
        for shard in groups[g]:
            @pl.when(z + 1 < n)
            def _():
                along(shard, z, 0, True).wait_send()

            @pl.when(z >= 1)
            def _():
                along(shard, z, 1, True).wait_send()

    def drain(d):
        def body(origin, up):
            for g in range(3):
                for shard in groups[g]:
                    if up:
                        @pl.when(z + 1 < n)
                        def _():
                            along(shard, origin, 0, False).wait_send()
                    else:
                        @pl.when(z >= 1)
                        def _():
                            along(shard, origin, 1, False).wait_send()
                    for kind in (2, 3, 4, 5):
                        across(shard, origin, kind).wait_send()

        both(d, body)

    loop(1, n, drain)


def on_device(n, hidden_in, norm_gain, query_weight, key_weight, value_weight, out_weight, slopes, block_choice):
    _, tokens, half_d = hidden_in.shape
    rows, width = query_weight.shape
    key_width = key_weight.shape[1]
    heads = width // HEAD_DIM
    local_blocks = block_choice.shape[1]
    blocks = n * local_blocks
    masked = blocks > NSEL

    def cut(w):
        return w.reshape(8, rows // 8, w.shape[1])

    operands = [
        hidden_in[0],
        norm_gain.reshape(half_d // 128, 128),
        cut(query_weight),
        cut(key_weight),
        cut(value_weight),
        cut(out_weight),
        slopes,
    ]
    vmem = pl.BlockSpec(memory_space=pltpu.VMEM)
    specs = [vmem] * 6 + [pl.BlockSpec(memory_space=pltpu.SMEM)]
    if masked:
        block = lax.axis_index("kv") * local_blocks + jnp.arange(local_blocks, dtype=jnp.int32)
        slot = jnp.arange(NSEL, dtype=jnp.int32)
        used = slot[None, :] < jnp.minimum(NSEL, block + 1)[:, None]
        names = jnp.arange(blocks, dtype=jnp.int32)
        hit = (block_choice[0][:, :, None] == names[None, None, :]) & used[:, :, None]
        bias = jnp.where(jnp.any(hit, axis=1), 0.0, NEG).astype(F32)
        bias = jnp.repeat(jnp.repeat(bias, BLOCK, axis=0), BLOCK, axis=1)
        operands.append(bias.reshape(tokens, n, tokens).swapaxes(0, 1))
        specs.append(vmem)
    dma = pltpu.SemaphoreType.DMA
    full = (n, 8, rows // 8)
    result = pl.pallas_call(
        functools.partial(kernel, n, masked),
        out_shape=jax.ShapeDtypeStruct((tokens // 2, n * rows), BF16),
        in_specs=specs,
        out_specs=vmem,
        scratch_shapes=[
            pltpu.VMEM((tokens, half_d), BF16),
            pltpu.VMEM((half_d // 128, 128), F32),
            pltpu.VMEM((n, tokens, rows), BF16),
            pltpu.VMEM((*full, width), BF16),
            pltpu.VMEM((*full, key_width), BF16),
            pltpu.VMEM((*full, key_width), BF16),
            pltpu.VMEM((*full, width), BF16),
            pltpu.VMEM((tokens, width), F32),
            pltpu.VMEM((tokens, key_width), F32),
            pltpu.VMEM((tokens, key_width), F32),
            pltpu.VMEM((heads, tokens, HEAD_DIM), BF16),
            pltpu.VMEM((n, tokens, key_width), BF16),
            pltpu.VMEM((n, tokens, key_width), BF16),
            pltpu.VMEM((heads, tokens, HEAD_DIM), F32),
            pltpu.VMEM((heads, tokens, HEAD_DIM), F32),
            pltpu.VMEM((heads, tokens, HEAD_DIM), F32),
            pltpu.VMEM((2, tokens // 2, width), BF16),
            pltpu.VMEM((n, tokens // 2, rows), BF16),
            pltpu.VMEM((n, tokens // 2, rows), BF16),
            pltpu.VMEM((n, tokens // 2, rows), BF16),
            dma((4, 6, n)),
            dma((4, 6, n)),
            dma((2, n)),
            dma((2, n)),
            dma((2,)),
            dma((2,)),
            dma((n,)),
            dma((n,)),
        ],
        compiler_params=pltpu.CompilerParams(collective_id=0, has_side_effects=True),
    )(*operands)
    return result[None]


def solution(mesh):
    in_specs = (
        P(("grp", "dp"), "kv", "tp"),
        P("tp"),
        P("kv", "tp"),
        P("kv", "tp"),
        P("kv", "tp"),
        P("kv", "tp"),
        P("tp"),
        P(("grp", "dp"), "kv", None),
    )
    out_specs = P(("grp", "dp"), ("kv", "tp"), None)
    return jax.shard_map(
        functools.partial(on_device, mesh.shape["kv"]),
        mesh=mesh,
        in_specs=in_specs,
        out_specs=out_specs,
        check_vma=False,
    )
```

```python
import functools

import jax
import jax.numpy as jnp
from jax import lax
from jax.experimental import pallas as pl
from jax.experimental.pallas import tpu as pltpu
from jax.sharding import PartitionSpec as P

HEAD_DIM = 128
BLOCK = 64
NSEL = 16
EPS = 1e-06
NEG = -1e30
ORDER = (
    ("own", 1, 1), ("own", 0, -1), ("own", 0, -3), ("norm", 0, 0), ("own", 0, 2), ("pass", 0, -1),
    ("own", 0, -2), ("own", 0, 1), ("pass", 1, 1), ("own", 0, 3), ("own", 1, -1), ("pass", 0, -2),
    ("pass", 0, 2), ("pass", 0, -3), ("pass", 0, 1), ("turn", 0, -1), ("pass", 1, -1), ("pass", 0, 3),
    ("turn", 1, 1), ("turn", 0, 2), ("own", 2, -1), ("turn", 0, 3), ("pass", 1, 2), ("own", 2, 1),
    ("turn", 0, -2), ("turn", 0, 1), ("pass", 1, 3), ("turn", 0, -3), ("use", 0, -1), ("pass", 1, -2),
    ("use", 0, 2), ("pass", 2, 1), ("pass", 2, -1), ("use", 0, 1), ("turn", 1, -2), ("pass", 1, -3),
    ("turn", 1, 3), ("use", 0, 3), ("use", 0, -3), ("use", 1, 1), ("pass", 2, 2), ("turn", 1, 2),
    ("pass", 2, 3), ("use", 0, -2), ("turn", 1, -1), ("keys", 0, 0), ("pass", 2, -2), ("turn", 1, -3),
    ("use", 1, 3), ("pass", 2, -3), ("use", 1, -1), ("turn", 2, 2), ("turn", 2, -1), ("turn", 2, 1),
    ("use", 1, -3), ("use", 1, -2), ("use", 1, 2), ("turn", 2, -2), ("chunk", 0, 0), ("chunk", 0, 1),
    ("turn", 2, 3), ("chunk", 0, 2), ("chunk", 0, 3), ("turn", 2, -3), ("out", 0, 0), ("use", 2, 3),
    ("use", 2, 1), ("use", 2, -2), ("use", 2, -1), ("use", 2, 2), ("use", 2, -3),
)
ROUTES = ("uni", "chain", "chain")
MESH = pl.DeviceIdType.MESH
BF16 = jnp.bfloat16
F32 = jnp.float32


def dot(a, b):
    return jnp.dot(a, b, preferred_element_type=F32)


def dot_t(a, b):
    return lax.dot_general(a, b, (((1,), (1,)), ((), ())), preferred_element_type=F32)


def loop(low, high, body):
    if high - low <= 4:
        for i in range(low, high):
            body(i)
    else:
        lax.fori_loop(low, high, lambda i, c: (body(i), c)[1], 0)


def kernel(n, masked, *refs):
    refs = list(refs)
    hid, gain, wq, wk, wv, wo, slopes = refs[:7]
    refs = refs[7:]
    mask = refs.pop(0) if masked else None
    (
        out, hid2, gain2, xn, fq, fk, fv, fo, qacc, kacc, vacc, qs, kall, vall,
        mrun, lrun, acc, att, pown, psend, precv,
        wsend, wrecv, zsend, ksend, krecv, hsend, hrecv, osend, orecv,
    ) = refs
    grp, dp = lax.axis_index("grp"), lax.axis_index("dp")
    z, tp = lax.axis_index("kv"), lax.axis_index("tp")
    xb, yb = lax.rem(dp, 2), lax.rem(grp, 2)
    col = 2 * yb + xb
    col_x, col_y, col_d = 2 * yb + 1 - xb, 2 * (1 - yb) + xb, 2 * (1 - yb) + 1 - xb
    x_id = (grp, dp + 1 - 2 * xb, z, tp)
    y_id = (grp + 1 - 2 * yb, dp, z, tp)
    sib = (grp, dp, z, 1 - tp)

    def at_z(other):
        return (grp, dp, other, tp)

    tokens, half_d = hid.shape
    heads = slopes.shape[0]
    rows = xn.shape[2]
    groups = (((wk, fk, 0), (wv, fv, 1)), ((wq, fq, 2),), ((wo, fo, 3),))

    barrier = pltpu.get_barrier_semaphore()
    for dev in (sib, x_id, y_id):
        pl.semaphore_signal(barrier, inc=1, device_id=dev, device_id_type=MESH)
    for d in range(1, n):
        pl.semaphore_signal(barrier, inc=1, device_id=at_z(lax.rem(z + d, n)), device_id_type=MESH)
    pl.semaphore_wait(barrier, n + 2)

    def remote(src, dst, send, recv, dev):
        return pltpu.make_async_remote_copy(
            src_ref=src, dst_ref=dst, send_sem=send, recv_sem=recv, device_id=dev, device_id_type=MESH
        )

    swap = [
        remote(hid, hid2, hsend.at[0], hrecv.at[0], sib),
        remote(gain, gain2, hsend.at[1], hrecv.at[1], sib),
    ]
    for copy in swap:
        copy.start()

    def along(shard, origin, step, act):
        w, f, a = shard
        part = pl.ds(2 * col, 2)
        src = w.at[part] if origin is z else f.at[origin, part]
        target = z + step

        @pl.when((target < n) & (target >= 0))
        def _():
            sem = lax.rem(target, n)
            act(remote(src, f.at[origin, part], zsend.at[a, sem, origin], wrecv.at[a, 0, origin], at_z(target)))

    def across(shard, origin, kind):
        _, f, a = shard
        part, dev = {
            2: (pl.ds(2 * col, 2), x_id),
            3: (pl.ds(2 * col, 2), y_id),
            4: (pl.ds(2 * col_x, 1), y_id),
            5: (pl.ds(2 * col_y + 1, 1), x_id),
        }[kind]
        ref = f.at[origin, part]
        return remote(ref, ref, wsend.at[a, kind, origin], wrecv.at[a, kind, origin], dev)

    def arrive(shard, origin, kind):
        _, f, a = shard
        part = {
            0: pl.ds(2 * col, 2),
            2: pl.ds(2 * col_x, 2),
            3: pl.ds(2 * col_y, 2),
            4: pl.ds(2 * col_d, 1),
            5: pl.ds(2 * col_d + 1, 1),
        }[kind]
        ref = f.at[origin, part]
        remote(ref, ref, wsend.at[a, kind, origin], wrecv.at[a, kind, origin], x_id).wait_recv()

    def start(copy):
        copy.start()

    def own_steps(g):
        far = {"uni": n - 1, "even": 2, "chain": 1}[ROUTES[g]]
        return [sign * d for d in range(1, far + 1) for sign in (1, -1)]

    def own(g, step, act):
        for shard in groups[g]:
            along(shard, z, step, act)

    def forwards(g, shard, origin, up, d, act):
        def go():
            for step in (1, 2) if ROUTES[g] == "even" else (1,):
                along(shard, origin, step if up else -step, act)

        if ROUTES[g] == "chain":
            go()
        elif ROUTES[g] == "even":
            if not isinstance(d, int):
                pl.when(lax.rem(d, 2) == 0)(go)
            elif d % 2 == 0:
                go()

    def one(d, up, body):
        if up:
            pl.when(z - d >= 0)(lambda: body(z - d, True))
        else:
            pl.when(z + d < n)(lambda: body(z + d, False))

    def both(d, body, ways=(True, False)):
        for up in ways:
            one(d, up, body)

    def step_a(g, d, ways=(True, False)):
        def body(origin, up):
            for shard in groups[g]:
                arrive(shard, origin, 0)
                forwards(g, shard, origin, up, d, start)
                across(shard, origin, 2).start()
                across(shard, origin, 3).start()

        both(d, body, ways)

    def step_b(g, d, ways=(True, False)):
        def body(origin, up):
            for shard in groups[g]:
                arrive(shard, origin, 2)
                across(shard, origin, 4).start()
                arrive(shard, origin, 3)
                across(shard, origin, 5).start()

        both(d, body, ways)

    def whole(f, origin):
        return f[origin].reshape(rows, f.shape[-1])

    def step_c(g, d, ways=(True, False)):
        def body(origin, up):
            for shard in groups[g]:
                arrive(shard, origin, 4)
                arrive(shard, origin, 5)
                if g < 2:
                    target = (kacc, vacc, qacc)[shard[2]]
                    target[...] += dot(xn[origin], whole(shard[1], origin))
                else:
                    project_out(origin, whole(fo, origin))

        both(d, body, ways)

    def norm():
        for copy in swap:
            copy.wait()
        lanes = HEAD_DIM
        square = jnp.zeros((tokens, lanes), F32)
        for ref in (hid, hid2):
            for j in range(half_d // lanes):
                piece = ref[:, j * lanes : (j + 1) * lanes].astype(F32)
                square = square + piece * piece
        inverse = lax.rsqrt(jnp.sum(square, axis=1, keepdims=True) / (2 * half_d) + EPS)
        for ref, g_ref, half in ((hid, gain, tp), (hid2, gain2, 1 - tp)):
            for j in range(half_d // lanes):
                piece = ref[:, j * lanes : (j + 1) * lanes].astype(F32)
                value = (piece * inverse * g_ref[j : j + 1, :]).astype(BF16)
                first = j * lanes
                xn[half * (n // 2) + first // rows, :, first % rows : first % rows + lanes] = value

        mine = xn[z]
        kacc[...] = dot(mine, wk[...].reshape(rows, -1))
        vacc[...] = dot(mine, wv[...].reshape(rows, -1))
        qacc[...] = dot(mine, wq[...].reshape(rows, -1))

    def key_copy(ref, i, d):
        return remote(ref.at[z], ref.at[z], ksend.at[i, d], krecv.at[i, z], at_z(z + d))

    def key_each(d, act):
        @pl.when(z + d < n)
        def _():
            for i, ref in enumerate((kall, vall)):
                act(key_copy(ref, i, d))

    def send_keys():
        kall[z] = kacc[...].astype(BF16)
        vall[z] = vacc[...].astype(BF16)
        loop(1, n, lambda d: key_each(d, start))

    scale = HEAD_DIM**-0.5
    qpos = lax.broadcasted_iota(jnp.int32, (tokens, tokens), 0)
    kpos = lax.broadcasted_iota(jnp.int32, (tokens, tokens), 1)

    def chunk(d, first):
        origin = z - d
        if not first:
            for i, ref in enumerate((kall, vall)):
                remote(ref.at[origin], ref.at[origin], ksend.at[i, d], krecv.at[i, origin], sib).wait_recv()
        else:
            for h in range(heads):
                qs[h] = qacc[:, h * HEAD_DIM : (h + 1) * HEAD_DIM].astype(BF16)
        keys, values = kall[origin], vall[origin]
        dist = jnp.abs(qpos - kpos + d * tokens).astype(F32) / BLOCK
        for h in range(heads):
            s = dot_t(qs[h], keys) * scale - slopes[h] * dist
            if masked:
                s = s + mask[origin]
            elif first:
                s = jnp.where(kpos // BLOCK <= qpos // BLOCK, s, NEG)
            top = jnp.max(s, axis=1, keepdims=True)
            if not first:
                before = mrun[h][:, :1]
                top = jnp.maximum(top, before)
                fade = jnp.exp(before - top)
            w = jnp.exp(s - top)
            total = jnp.sum(w, axis=1, keepdims=True)
            summed = dot(w.astype(BF16), values)
            if not first:
                total = total + lrun[h][:, :1] * fade
                summed = summed + acc[h] * fade
            mrun[h] = jnp.broadcast_to(top, (tokens, HEAD_DIM))
            lrun[h] = jnp.broadcast_to(total, (tokens, HEAD_DIM))
            acc[h] = summed

    def out_copy(origin):
        return remote(psend.at[origin], precv.at[origin], osend.at[origin], orecv.at[origin], sib)

    def project_out(origin, weight):
        psend[origin] = dot_t(att[1 - tp], weight).astype(BF16)
        out_copy(origin).start()
        pown[origin] = dot_t(att[tp], weight).astype(BF16)

    def start_out():
        half = tokens // 2
        for h in range(heads):
            value = (acc[h] / lrun[h]).astype(BF16)
            att[:, :, h * HEAD_DIM : (h + 1) * HEAD_DIM] = value.reshape(2, half, HEAD_DIM)
        project_out(z, wo[...].reshape(rows, -1))

    def later_chunk(d):
        pl.when(z - d >= 0)(lambda: chunk(d, False))

    if n == 4:
        for step, g, d in ORDER:
            if step == "own":
                own(g, d, start)
            elif step in ("pass", "turn", "use"):
                {"pass": step_a, "turn": step_b, "use": step_c}[step](g, abs(d), (d > 0,))
            elif step == "chunk":
                later_chunk(d) if d else chunk(0, True)
            else:
                {"norm": norm, "keys": send_keys, "out": start_out}[step]()
    else:
        for g in range(3):
            for step in own_steps(g):
                own(g, step, start)
        norm()
        for g, then in ((0, send_keys), (1, lambda: chunk(0, True))):
            loop(1, n, lambda d: step_a(g, d))
            loop(1, n, lambda d: step_b(g, d))
            loop(1, n, lambda d: step_c(g, d))
            then()
        loop(1, n, lambda d: step_a(2, d))
        loop(1, n, lambda d: step_b(2, d))
        loop(1, n, later_chunk)
        start_out()
        loop(1, n, lambda d: step_c(2, d))

    def finish(origin):
        out_copy(origin).wait()
        value = pown[origin].astype(F32) + precv[origin].astype(F32)
        first = origin * rows
        if not isinstance(origin, int):
            first = pl.multiple_of(first, rows)
        out[:, pl.ds(first, rows)] = value.astype(BF16)

    finish(z)
    loop(1, n, lambda d: both(d, lambda origin, up: finish(origin)))

    def left(copy):
        copy.wait_send()

    loop(1, n, lambda d: key_each(d, left))
    for g in range(3):
        for step in own_steps(g):
            own(g, step, left)

    def drain(d):
        def body(origin, up):
            for g in range(3):
                for shard in groups[g]:
                    forwards(g, shard, origin, up, d, left)
                    for kind in (2, 3, 4, 5):
                        across(shard, origin, kind).wait_send()

        both(d, body)

    loop(1, n, drain)


def on_device(n, hidden_in, norm_gain, query_weight, key_weight, value_weight, out_weight, slopes, block_choice):
    _, tokens, half_d = hidden_in.shape
    rows, width = query_weight.shape
    key_width = key_weight.shape[1]
    heads = width // HEAD_DIM
    local_blocks = block_choice.shape[1]
    blocks = n * local_blocks
    masked = blocks > NSEL

    def cut(w):
        return w.reshape(8, rows // 8, w.shape[1])

    operands = [
        hidden_in[0],
        norm_gain.reshape(half_d // 128, 128),
        cut(query_weight),
        cut(key_weight),
        cut(value_weight),
        cut(out_weight),
        slopes,
    ]
    vmem = pl.BlockSpec(memory_space=pltpu.VMEM)
    specs = [vmem] * 6 + [pl.BlockSpec(memory_space=pltpu.SMEM)]
    if masked:
        block = lax.axis_index("kv") * local_blocks + jnp.arange(local_blocks, dtype=jnp.int32)
        slot = jnp.arange(NSEL, dtype=jnp.int32)
        used = slot[None, :] < jnp.minimum(NSEL, block + 1)[:, None]
        names = jnp.arange(blocks, dtype=jnp.int32)
        hit = (block_choice[0][:, :, None] == names[None, None, :]) & used[:, :, None]
        bias = jnp.where(jnp.any(hit, axis=1), 0.0, NEG).astype(F32)
        bias = jnp.repeat(jnp.repeat(bias, BLOCK, axis=0), BLOCK, axis=1)
        operands.append(bias.reshape(tokens, n, tokens).swapaxes(0, 1))
        specs.append(vmem)
    dma = pltpu.SemaphoreType.DMA
    full = (n, 8, rows // 8)
    result = pl.pallas_call(
        functools.partial(kernel, n, masked),
        out_shape=jax.ShapeDtypeStruct((tokens // 2, n * rows), BF16),
        in_specs=specs,
        out_specs=vmem,
        scratch_shapes=[
            pltpu.VMEM((tokens, half_d), BF16),
            pltpu.VMEM((half_d // 128, 128), F32),
            pltpu.VMEM((n, tokens, rows), BF16),
            pltpu.VMEM((*full, width), BF16),
            pltpu.VMEM((*full, key_width), BF16),
            pltpu.VMEM((*full, key_width), BF16),
            pltpu.VMEM((*full, width), BF16),
            pltpu.VMEM((tokens, width), F32),
            pltpu.VMEM((tokens, key_width), F32),
            pltpu.VMEM((tokens, key_width), F32),
            pltpu.VMEM((heads, tokens, HEAD_DIM), BF16),
            pltpu.VMEM((n, tokens, key_width), BF16),
            pltpu.VMEM((n, tokens, key_width), BF16),
            pltpu.VMEM((heads, tokens, HEAD_DIM), F32),
            pltpu.VMEM((heads, tokens, HEAD_DIM), F32),
            pltpu.VMEM((heads, tokens, HEAD_DIM), F32),
            pltpu.VMEM((2, tokens // 2, width), BF16),
            pltpu.VMEM((n, tokens // 2, rows), BF16),
            pltpu.VMEM((n, tokens // 2, rows), BF16),
            pltpu.VMEM((n, tokens // 2, rows), BF16),
            dma((4, 6, n)),
            dma((4, 6, n)),
            dma((4, n, n)),
            dma((2, n)),
            dma((2, n)),
            dma((2,)),
            dma((2,)),
            dma((n,)),
            dma((n,)),
        ],
        compiler_params=pltpu.CompilerParams(collective_id=0, has_side_effects=True),
    )(*operands)
    return result[None]


def solution(mesh):
    in_specs = (
        P(("grp", "dp"), "kv", "tp"),
        P("tp"),
        P("kv", "tp"),
        P("kv", "tp"),
        P("kv", "tp"),
        P("kv", "tp"),
        P("tp"),
        P(("grp", "dp"), "kv", None),
    )
    out_specs = P(("grp", "dp"), ("kv", "tp"), None)
    return jax.shard_map(
        functools.partial(on_device, mesh.shape["kv"]),
        mesh=mesh,
        in_specs=in_specs,
        out_specs=out_specs,
        check_vma=False,
    )
```

```python
import functools

import jax
import jax.numpy as jnp
from jax import lax
from jax.experimental import pallas as pl
from jax.experimental.pallas import tpu as pltpu
from jax.sharding import PartitionSpec as P

HEAD_DIM = 128
BLOCK = 64
NSEL = 16
EPS = 1e-06
NEG = -1e30
ORDER = (
    ("own", 0, -1), ("own", 1, -1), ("own", 0, 1), ("own", 1, 1), ("pass", 0, -1), ("pass", 0, 1),
    ("pass", 0, -2), ("pass", 1, 1), ("pass", 1, -1), ("norm", 0, 0), ("own", 2, 1), ("own", 2, -1),
    ("pass", 0, 2), ("turn", 0, -1), ("pass", 0, -3), ("turn", 0, 1), ("pass", 1, 2), ("turn", 0, 2),
    ("turn", 0, -2), ("pass", 2, 1), ("pass", 1, -2), ("turn", 0, -3), ("turn", 1, -1), ("pass", 0, 3),
    ("use", 0, -1), ("pass", 2, -1), ("pass", 1, -3), ("use", 0, 1), ("use", 0, 2), ("use", 0, -2),
    ("pass", 1, 3), ("turn", 0, 3), ("turn", 1, 2), ("turn", 1, 1), ("turn", 1, 3), ("pass", 2, 2),
    ("use", 0, 3), ("pass", 2, 3), ("use", 0, -3), ("pass", 2, -2), ("keys", 0, 0), ("turn", 1, -2),
    ("turn", 1, -3), ("use", 1, 1), ("pass", 2, -3), ("turn", 2, -1), ("use", 1, 2), ("use", 1, -3),
    ("use", 1, -1), ("turn", 2, -2), ("use", 1, -2), ("turn", 2, 1), ("use", 1, 3), ("chunk", 0, 0),
    ("chunk", 0, 1), ("turn", 2, 2), ("turn", 2, 3), ("chunk", 0, 2), ("turn", 2, -3), ("chunk", 0, 3),
    ("out", 0, 0), ("use", 2, 1), ("use", 2, -2), ("use", 2, -1), ("use", 2, 3), ("use", 2, 2),
    ("use", 2, -3),
)
ROUTES = ("chain", "chain", "chain")
MESH = pl.DeviceIdType.MESH
BF16 = jnp.bfloat16
F32 = jnp.float32


def dot(a, b):
    return jnp.dot(a, b, preferred_element_type=F32)


def dot_t(a, b):
    return lax.dot_general(a, b, (((1,), (1,)), ((), ())), preferred_element_type=F32)


def loop(low, high, body):
    if high - low <= 4:
        for i in range(low, high):
            body(i)
    else:
        lax.fori_loop(low, high, lambda i, c: (body(i), c)[1], 0)


def kernel(n, masked, *refs):
    refs = list(refs)
    hid, gain, wq, wk, wv, wo, slopes = refs[:7]
    refs = refs[7:]
    mask = refs.pop(0) if masked else None
    (
        out, hid2, gain2, xn, fq, fk, fv, fo, qacc, kacc, vacc, qs, kall, vall,
        mrun, lrun, acc, att, pown, psend, precv,
        wsend, wrecv, zsend, ksend, krecv, hsend, hrecv, osend, orecv,
    ) = refs
    grp, dp = lax.axis_index("grp"), lax.axis_index("dp")
    z, tp = lax.axis_index("kv"), lax.axis_index("tp")
    xb, yb = lax.rem(dp, 2), lax.rem(grp, 2)
    col = 2 * yb + xb
    col_x, col_y, col_d = 2 * yb + 1 - xb, 2 * (1 - yb) + xb, 2 * (1 - yb) + 1 - xb
    x_id = (grp, dp + 1 - 2 * xb, z, tp)
    y_id = (grp + 1 - 2 * yb, dp, z, tp)
    sib = (grp, dp, z, 1 - tp)

    def at_z(other):
        return (grp, dp, other, tp)

    tokens, half_d = hid.shape
    heads = slopes.shape[0]
    rows = xn.shape[2]
    groups = (((wk, fk, 0), (wv, fv, 1)), ((wq, fq, 2),), ((wo, fo, 3),))

    barrier = pltpu.get_barrier_semaphore()
    for dev in (sib, x_id, y_id):
        pl.semaphore_signal(barrier, inc=1, device_id=dev, device_id_type=MESH)
    for d in range(1, n):
        pl.semaphore_signal(barrier, inc=1, device_id=at_z(lax.rem(z + d, n)), device_id_type=MESH)
    pl.semaphore_wait(barrier, n + 2)

    def remote(src, dst, send, recv, dev):
        return pltpu.make_async_remote_copy(
            src_ref=src, dst_ref=dst, send_sem=send, recv_sem=recv, device_id=dev, device_id_type=MESH
        )

    swap = [
        remote(hid, hid2, hsend.at[0], hrecv.at[0], sib),
        remote(gain, gain2, hsend.at[1], hrecv.at[1], sib),
    ]
    for copy in swap:
        copy.start()

    def along(shard, origin, step, act):
        w, f, a = shard
        part = pl.ds(2 * col, 2)
        src = w.at[part] if origin is z else f.at[origin, part]
        target = z + step

        @pl.when((target < n) & (target >= 0))
        def _():
            sem = lax.rem(target, n)
            act(remote(src, f.at[origin, part], zsend.at[a, sem, origin], wrecv.at[a, 0, origin], at_z(target)))

    def across(shard, origin, kind):
        _, f, a = shard
        part, dev = {
            2: (pl.ds(2 * col, 2), x_id),
            3: (pl.ds(2 * col, 2), y_id),
            4: (pl.ds(2 * col_x, 1), y_id),
            5: (pl.ds(2 * col_y + 1, 1), x_id),
        }[kind]
        ref = f.at[origin, part]
        return remote(ref, ref, wsend.at[a, kind, origin], wrecv.at[a, kind, origin], dev)

    def arrive(shard, origin, kind):
        _, f, a = shard
        part = {
            0: pl.ds(2 * col, 2),
            2: pl.ds(2 * col_x, 2),
            3: pl.ds(2 * col_y, 2),
            4: pl.ds(2 * col_d, 1),
            5: pl.ds(2 * col_d + 1, 1),
        }[kind]
        ref = f.at[origin, part]
        remote(ref, ref, wsend.at[a, kind, origin], wrecv.at[a, kind, origin], x_id).wait_recv()

    def start(copy):
        copy.start()

    def own_steps(g):
        far = {"uni": n - 1, "even": 2, "chain": 1}[ROUTES[g]]
        return [sign * d for d in range(1, far + 1) for sign in (1, -1)]

    def own(g, step, act):
        for shard in groups[g]:
            along(shard, z, step, act)

    def forwards(g, shard, origin, up, d, act):
        def go():
            for step in (1, 2) if ROUTES[g] == "even" else (1,):
                along(shard, origin, step if up else -step, act)

        if ROUTES[g] == "chain":
            go()
        elif ROUTES[g] == "even":
            if not isinstance(d, int):
                pl.when(lax.rem(d, 2) == 0)(go)
            elif d % 2 == 0:
                go()

    def one(d, up, body):
        if up:
            pl.when(z - d >= 0)(lambda: body(z - d, True))
        else:
            pl.when(z + d < n)(lambda: body(z + d, False))

    def both(d, body, ways=(True, False)):
        for up in ways:
            one(d, up, body)

    def step_a(g, d, ways=(True, False)):
        def body(origin, up):
            for shard in groups[g]:
                arrive(shard, origin, 0)
                forwards(g, shard, origin, up, d, start)
                across(shard, origin, 2).start()
                across(shard, origin, 3).start()

        both(d, body, ways)

    def step_b(g, d, ways=(True, False)):
        def body(origin, up):
            for shard in groups[g]:
                arrive(shard, origin, 2)
                across(shard, origin, 4).start()
                arrive(shard, origin, 3)
                across(shard, origin, 5).start()

        both(d, body, ways)

    def whole(f, origin):
        return f[origin].reshape(rows, f.shape[-1])

    def step_c(g, d, ways=(True, False)):
        def body(origin, up):
            for shard in groups[g]:
                arrive(shard, origin, 4)
                arrive(shard, origin, 5)
                if g < 2:
                    target = (kacc, vacc, qacc)[shard[2]]
                    target[...] += dot(xn[origin], whole(shard[1], origin))
                else:
                    project_out(origin, whole(fo, origin))

        both(d, body, ways)

    def norm():
        for copy in swap:
            copy.wait()
        lanes = HEAD_DIM
        square = jnp.zeros((tokens, lanes), F32)
        for ref in (hid, hid2):
            for j in range(half_d // lanes):
                piece = ref[:, j * lanes : (j + 1) * lanes].astype(F32)
                square = square + piece * piece
        inverse = lax.rsqrt(jnp.sum(square, axis=1, keepdims=True) / (2 * half_d) + EPS)
        for ref, g_ref, half in ((hid, gain, tp), (hid2, gain2, 1 - tp)):
            for j in range(half_d // lanes):
                piece = ref[:, j * lanes : (j + 1) * lanes].astype(F32)
                value = (piece * inverse * g_ref[j : j + 1, :]).astype(BF16)
                first = j * lanes
                xn[half * (n // 2) + first // rows, :, first % rows : first % rows + lanes] = value

        mine = xn[z]
        kacc[...] = dot(mine, wk[...].reshape(rows, -1))
        vacc[...] = dot(mine, wv[...].reshape(rows, -1))
        qacc[...] = dot(mine, wq[...].reshape(rows, -1))

    def key_copy(ref, i, d):
        return remote(ref.at[z], ref.at[z], ksend.at[i, d], krecv.at[i, z], at_z(z + d))

    def key_each(d, act):
        @pl.when(z + d < n)
        def _():
            for i, ref in enumerate((kall, vall)):
                act(key_copy(ref, i, d))

    def send_keys():
        kall[z] = kacc[...].astype(BF16)
        vall[z] = vacc[...].astype(BF16)
        loop(1, n, lambda d: key_each(d, start))

    scale = HEAD_DIM**-0.5
    qpos = lax.broadcasted_iota(jnp.int32, (tokens, tokens), 0)
    kpos = lax.broadcasted_iota(jnp.int32, (tokens, tokens), 1)

    def chunk(d, first):
        origin = z - d
        if not first:
            for i, ref in enumerate((kall, vall)):
                remote(ref.at[origin], ref.at[origin], ksend.at[i, d], krecv.at[i, origin], sib).wait_recv()
        else:
            for h in range(heads):
                qs[h] = qacc[:, h * HEAD_DIM : (h + 1) * HEAD_DIM].astype(BF16)
        keys, values = kall[origin], vall[origin]
        dist = jnp.abs(qpos - kpos + d * tokens).astype(F32) / BLOCK
        for h in range(heads):
            s = dot_t(qs[h], keys) * scale - slopes[h] * dist
            if masked:
                s = s + mask[origin]
            elif first:
                s = jnp.where(kpos // BLOCK <= qpos // BLOCK, s, NEG)
            top = jnp.max(s, axis=1, keepdims=True)
            if not first:
                before = mrun[h][:, :1]
                top = jnp.maximum(top, before)
                fade = jnp.exp(before - top)
            w = jnp.exp(s - top)
            total = jnp.sum(w, axis=1, keepdims=True)
            summed = dot(w.astype(BF16), values)
            if not first:
                total = total + lrun[h][:, :1] * fade
                summed = summed + acc[h] * fade
            mrun[h] = jnp.broadcast_to(top, (tokens, HEAD_DIM))
            lrun[h] = jnp.broadcast_to(total, (tokens, HEAD_DIM))
            acc[h] = summed

    def out_copy(origin):
        return remote(psend.at[origin], precv.at[origin], osend.at[origin], orecv.at[origin], sib)

    def project_out(origin, weight):
        psend[origin] = dot_t(att[1 - tp], weight).astype(BF16)
        out_copy(origin).start()
        pown[origin] = dot_t(att[tp], weight).astype(BF16)

    def start_out():
        half = tokens // 2
        for h in range(heads):
            value = (acc[h] / lrun[h]).astype(BF16)
            att[:, :, h * HEAD_DIM : (h + 1) * HEAD_DIM] = value.reshape(2, half, HEAD_DIM)
        project_out(z, wo[...].reshape(rows, -1))

    def later_chunk(d):
        pl.when(z - d >= 0)(lambda: chunk(d, False))

    if n == 4:
        for step, g, d in ORDER:
            if step == "own":
                own(g, d, start)
            elif step in ("pass", "turn", "use"):
                {"pass": step_a, "turn": step_b, "use": step_c}[step](g, abs(d), (d > 0,))
            elif step == "chunk":
                later_chunk(d) if d else chunk(0, True)
            else:
                {"norm": norm, "keys": send_keys, "out": start_out}[step]()
    else:
        for g in range(3):
            for step in own_steps(g):
                own(g, step, start)
        norm()
        for g, then in ((0, send_keys), (1, lambda: chunk(0, True))):
            loop(1, n, lambda d: step_a(g, d))
            loop(1, n, lambda d: step_b(g, d))
            loop(1, n, lambda d: step_c(g, d))
            then()
        loop(1, n, lambda d: step_a(2, d))
        loop(1, n, lambda d: step_b(2, d))
        loop(1, n, later_chunk)
        start_out()
        loop(1, n, lambda d: step_c(2, d))

    def finish(origin):
        out_copy(origin).wait()
        value = pown[origin].astype(F32) + precv[origin].astype(F32)
        first = origin * rows
        if not isinstance(origin, int):
            first = pl.multiple_of(first, rows)
        out[:, pl.ds(first, rows)] = value.astype(BF16)

    finish(z)
    loop(1, n, lambda d: both(d, lambda origin, up: finish(origin)))

    def left(copy):
        copy.wait_send()

    loop(1, n, lambda d: key_each(d, left))
    for g in range(3):
        for step in own_steps(g):
            own(g, step, left)

    def drain(d):
        def body(origin, up):
            for g in range(3):
                for shard in groups[g]:
                    forwards(g, shard, origin, up, d, left)
                    for kind in (2, 3, 4, 5):
                        across(shard, origin, kind).wait_send()

        both(d, body)

    loop(1, n, drain)


def on_device(n, hidden_in, norm_gain, query_weight, key_weight, value_weight, out_weight, slopes, block_choice):
    _, tokens, half_d = hidden_in.shape
    rows, width = query_weight.shape
    key_width = key_weight.shape[1]
    heads = width // HEAD_DIM
    local_blocks = block_choice.shape[1]
    blocks = n * local_blocks
    masked = blocks > NSEL

    def cut(w):
        return w.reshape(8, rows // 8, w.shape[1])

    operands = [
        hidden_in[0],
        norm_gain.reshape(half_d // 128, 128),
        cut(query_weight),
        cut(key_weight),
        cut(value_weight),
        cut(out_weight),
        slopes,
    ]
    vmem = pl.BlockSpec(memory_space=pltpu.VMEM)
    specs = [vmem] * 6 + [pl.BlockSpec(memory_space=pltpu.SMEM)]
    if masked:
        block = lax.axis_index("kv") * local_blocks + jnp.arange(local_blocks, dtype=jnp.int32)
        slot = jnp.arange(NSEL, dtype=jnp.int32)
        used = slot[None, :] < jnp.minimum(NSEL, block + 1)[:, None]
        names = jnp.arange(blocks, dtype=jnp.int32)
        hit = (block_choice[0][:, :, None] == names[None, None, :]) & used[:, :, None]
        bias = jnp.where(jnp.any(hit, axis=1), 0.0, NEG).astype(F32)
        bias = jnp.repeat(jnp.repeat(bias, BLOCK, axis=0), BLOCK, axis=1)
        operands.append(bias.reshape(tokens, n, tokens).swapaxes(0, 1))
        specs.append(vmem)
    dma = pltpu.SemaphoreType.DMA
    full = (n, 8, rows // 8)
    result = pl.pallas_call(
        functools.partial(kernel, n, masked),
        out_shape=jax.ShapeDtypeStruct((tokens // 2, n * rows), BF16),
        in_specs=specs,
        out_specs=vmem,
        scratch_shapes=[
            pltpu.VMEM((tokens, half_d), BF16),
            pltpu.VMEM((half_d // 128, 128), F32),
            pltpu.VMEM((n, tokens, rows), BF16),
            pltpu.VMEM((*full, width), BF16),
            pltpu.VMEM((*full, key_width), BF16),
            pltpu.VMEM((*full, key_width), BF16),
            pltpu.VMEM((*full, width), BF16),
            pltpu.VMEM((tokens, width), F32),
            pltpu.VMEM((tokens, key_width), F32),
            pltpu.VMEM((tokens, key_width), F32),
            pltpu.VMEM((heads, tokens, HEAD_DIM), BF16),
            pltpu.VMEM((n, tokens, key_width), BF16),
            pltpu.VMEM((n, tokens, key_width), BF16),
            pltpu.VMEM((heads, tokens, HEAD_DIM), F32),
            pltpu.VMEM((heads, tokens, HEAD_DIM), F32),
            pltpu.VMEM((heads, tokens, HEAD_DIM), F32),
            pltpu.VMEM((2, tokens // 2, width), BF16),
            pltpu.VMEM((n, tokens // 2, rows), BF16),
            pltpu.VMEM((n, tokens // 2, rows), BF16),
            pltpu.VMEM((n, tokens // 2, rows), BF16),
            dma((4, 6, n)),
            dma((4, 6, n)),
            dma((4, n, n)),
            dma((2, n)),
            dma((2, n)),
            dma((2,)),
            dma((2,)),
            dma((n,)),
            dma((n,)),
        ],
        compiler_params=pltpu.CompilerParams(collective_id=0, has_side_effects=True),
    )(*operands)
    return result[None]


def solution(mesh):
    in_specs = (
        P(("grp", "dp"), "kv", "tp"),
        P("tp"),
        P("kv", "tp"),
        P("kv", "tp"),
        P("kv", "tp"),
        P("kv", "tp"),
        P("tp"),
        P(("grp", "dp"), "kv", None),
    )
    out_specs = P(("grp", "dp"), ("kv", "tp"), None)
    return jax.shard_map(
        functools.partial(on_device, mesh.shape["kv"]),
        mesh=mesh,
        in_specs=in_specs,
        out_specs=out_specs,
        check_vma=False,
    )
```
